32 devices in a mesh: sp: 4 (over y, x), tp: 8 (over z, core).
Axes of the slice: x: 2, y: 2, z: 4, core: 2. Of those that a mesh axis runs over, the one named last changes fastest.
Arguments:
- tokens: bfloat16 [512, 1024], P('sp', 'tp'), may hold values from -6 to 6
- segment_ids: int32 [512], P('sp'), may hold values from 0 to 7, never falling along the last dimension, each value on 1 to 128 neighbouring positions
- gains: float32 [2, 1024], replicated, may hold values from 0.1 to 1.9
- w_query: bfloat16 [2, 1024, 1024], P(None, 'sp', 'tp'), may hold values from -0.1875 to 0.1875
- w_key: bfloat16 [2, 1024, 1024], P(None, 'sp', 'tp'), may hold values from -0.1875 to 0.1875
- w_value: bfloat16 [2, 1024, 1024], P(None, 'sp', 'tp'), may hold values from -0.1875 to 0.1875
- w_out: bfloat16 [2, 1024, 1024], P(None, 'tp', 'sp'), may hold values from -0.1875 to 0.1875
- rel_bias: float32 [2, 16, 5, 9], P(None, 'tp'), may hold values from -4 to 4
Outputs:
- mixed_out: bfloat16 [512, 1024], P('sp', 'tp')
The draws below stay inside these ranges and needn't reach their ends.
Inputs may be any that keep to these rules, and one draw needn't show every extreme that they name: `segment_ids`: segment numbers never fall along the token order; each document has 1 to 128 positions.
All inputs are finite; a program needn't handle non-finite values.
Results may differ from the reference program's by a relative error of at most 0.03.
Values may be sent and summed in bfloat16 or wider, within the bound.
A program may use at most 64 MiB of HBM per device.

```python
import math
import jax
import jax.numpy as jnp
import numpy as np
from jax import lax

HEADS = 16
HEAD_DIM = 64
D = 1024
GRID_W = 32
ROWS_DEV = 4
REACH_R = 2
REACH_C = 4
LAYERS = 2
TOKENS = 512
N_SP = 4


def block_levels(own_key, extent, split, smallest, high):
    def one(dim, parts):
        steps = jax.random.uniform(jax.random.fold_in(jax.random.fold_in(own_key, 6), dim), (parts,), jnp.float32, smallest / len(split), high / len(split))
        return jnp.repeat(jnp.exp(steps), extent[dim] // parts).reshape((-1,) + (1,) * (len(extent) - dim - 1))

    level = one(*split[0])
    for cut in split[1:]:
        level = level * one(*cut)
    return level


def profile(amount, total, most, skew):
    portions = [(1 << 20) // math.isqrt(grade ** skew) + 1 for grade in range(2, amount + 1)]
    surplus, counts = total - most - (amount - 1), [1] * (amount - 1)
    while surplus > 0:
        candidates = [i for i in range(amount - 1) if counts[i] < most]
        pool, remaining = sum([portions[i] for i in candidates]), surplus
        for i in candidates:
            extra = min(most - counts[i], max(1, remaining * portions[i] // pool), surplus)
            counts[i] = counts[i] + extra
            surplus = surplus - extra
    return np.array([most] + counts)


def uneven_parts(own_key, number_of, total, limit, slope):
    if number_of == 2:
        one = jax.random.randint(own_key, (), max(1, total - limit), min(limit, total - 1) + 1)
        return jnp.stack([one, total - one])
    lengths = jnp.asarray(profile(number_of, total, limit, slope), jnp.int32)
    couples = (number_of - 1) // 2
    donor, sink = lengths[1:1 + 2 * couples:2], lengths[2:2 + 2 * couples:2]
    margin = jnp.minimum(donor - 1, limit - sink)
    moved = jax.random.randint(jax.random.fold_in(own_key, 1), (couples,), 0, 1 << 20) % (margin + 1)
    lengths = lengths.at[1:1 + 2 * couples:2].set(donor - moved).at[2:2 + 2 * couples:2].set(sink + moved)
    return lengths[jax.random.permutation(jax.random.fold_in(own_key, 2), number_of)]


def noise(own_key, shape, deviation, bound, split=(), kind=jnp.bfloat16):
    gain = block_levels(own_key, shape, split, -0.22, 0.18) if split else 1.0
    array = jax.random.normal(own_key, shape, jnp.float32) * deviation * gain
    return jnp.minimum(jnp.maximum(array, -bound), bound).astype(kind)


def setup_inputs(seed: int = 0) -> dict:
    arg_keys = jax.random.split(jax.random.key(seed), 9)
    tokens = noise(arg_keys[0], (TOKENS, D), 1.0, 6.0, ((0, 4), (1, 8)))
    segment_ids = jnp.searchsorted(jnp.cumsum(uneven_parts(arg_keys[1], 2 * N_SP, TOKENS, ROWS_DEV * GRID_W, 1)), jnp.arange(TOKENS), side="right").astype(jnp.int32)
    gains = jnp.clip(1.0 + 0.18 * jax.random.normal(arg_keys[2], (LAYERS, D), jnp.float32), 0.1, 1.9)
    w_query = noise(arg_keys[3], (LAYERS, D, D), D ** -0.5, 0.1875, ((1, 4), (2, 8)))
    w_key = noise(arg_keys[4], (LAYERS, D, D), D ** -0.5, 0.1875, ((1, 4), (2, 8)))
    w_value = noise(arg_keys[5], (LAYERS, D, D), D ** -0.5, 0.1875, ((1, 4), (2, 8)))
    w_out = noise(arg_keys[6], (LAYERS, D, D), D ** -0.5, 0.1875, ((1, 8), (2, 4)))
    rel_bias = noise(arg_keys[7], (LAYERS, HEADS, 2 * REACH_R + 1, 2 * REACH_C + 1), 1.0, 4.0, ((1, 8),), jnp.float32)
    return dict(tokens=tokens, segment_ids=segment_ids, gains=gains, w_query=w_query, w_key=w_key, w_value=w_value, w_out=w_out, rel_bias=rel_bias)


norm_eps = 1e-06
masked_score = -1e+30

def normalize(features, gain_row):
    feat32 = features.astype(jnp.float32)
    mean_sq = lax.optimization_barrier(jnp.mean(feat32 * feat32, axis=-1, keepdims=True))
    return (feat32 * lax.rsqrt(mean_sq + norm_eps) * gain_row).astype(jnp.bfloat16)

def attend(query_rows, key_rows, value_rows, doc_query, doc_keys, bias_table, reach_r, reach_c):
    row_count = query_rows.shape[0]
    col_count = query_rows.shape[1]
    key_pad = jnp.pad(key_rows, ((0, 0), (reach_c, reach_c), (0, 0), (0, 0)))
    value_pad = jnp.pad(value_rows, ((0, 0), (reach_c, reach_c), (0, 0), (0, 0)))
    doc_pad = jnp.pad(doc_keys, ((0, 0), (reach_c, reach_c)), constant_values=-1)
    score_scale = query_rows.shape[-1] ** (-0.5)
    query32 = query_rows.astype(jnp.float32) * score_scale
    score_list = []
    offsets = []
    for row_off in range(2 * reach_r + 1):
        for col_off in range(2 * reach_c + 1):
            key_part = key_pad[row_off:row_off + row_count, col_off:col_off + col_count].astype(jnp.float32)
            raw_score = lax.optimization_barrier(jnp.sum(query32 * key_part, axis=-1)) + bias_table[:, row_off, col_off]
            same_doc = doc_pad[row_off:row_off + row_count, col_off:col_off + col_count] == doc_query
            score_list.append(jnp.where(same_doc[..., None], raw_score, masked_score))
            offsets.append((row_off, col_off))
    scores = jnp.stack(score_list)
    score_peak = lax.optimization_barrier(jnp.max(scores, axis=0))
    weights = jnp.exp(scores - score_peak)
    denominator = lax.optimization_barrier(jnp.sum(weights, axis=0))
    blended = jnp.zeros(query_rows.shape, jnp.float32)
    for position, (row_off, col_off) in enumerate(offsets):
        value_part = value_pad[row_off:row_off + row_count, col_off:col_off + col_count].astype(jnp.float32)
        blended = blended + weights[position][..., None] * value_part
    return (blended / denominator[..., None]).astype(jnp.bfloat16)

def project(normed, weight, row_count):
    result = jnp.dot(normed, weight, preferred_element_type=jnp.float32).astype(jnp.bfloat16)
    return result.reshape(row_count, GRID_W, -1, HEAD_DIM)

def reference(tokens, segment_ids, gains, w_query, w_key, w_value, w_out, rel_bias):
    grid_rows = ROWS_DEV * N_SP
    doc_grid = segment_ids.reshape(grid_rows, GRID_W)
    doc_ext = jnp.pad(doc_grid, ((REACH_R, REACH_R), (0, 0)), constant_values=-1)
    row_pad = ((REACH_R, REACH_R), (0, 0), (0, 0), (0, 0))
    current = tokens
    for layer_index in range(LAYERS):
        normed = normalize(current, gains[layer_index])
        query_rows = project(normed, w_query[layer_index], grid_rows)
        key_rows = jnp.pad(project(normed, w_key[layer_index], grid_rows), row_pad)
        value_rows = jnp.pad(project(normed, w_value[layer_index], grid_rows), row_pad)
        attended = attend(query_rows, key_rows, value_rows, doc_grid, doc_ext, rel_bias[layer_index], REACH_R, REACH_C).reshape(TOKENS, D)
        current = jnp.dot(attended, w_out[layer_index], preferred_element_type=jnp.float32).astype(jnp.bfloat16)
    return current
```

```python
import functools

import jax
import jax.numpy as jnp
from jax import lax
from jax.experimental import pallas as pl
from jax.experimental.pallas import tpu as pltpu
from jax.sharding import PartitionSpec as P

MESH = pl.DeviceIdType.MESH

HEAD_DIM = 64
GRID_W = 32
REACH_R = 2
REACH_C = 4

norm_eps = 1e-06
masked_score = -1e30
F32 = jnp.float32
BF16 = jnp.bfloat16


def remote(src, dst, send_sem, recv_sem, where):
    return pltpu.make_async_remote_copy(
        src_ref=src, dst_ref=dst, send_sem=send_sem, recv_sem=recv_sem, device_id=where, device_id_type=MESH
    )


def kernel(
    n_sp, n_tp, tok, seg, gains, wq, wk, wv, wo, rel, out,
    xbuf, wbuf, wobuf, kvbuf, part, rsbuf, cur, docbuf, gbuf, relbuf, biasbuf,
    local_sem, x_send, x_recv, w_send, w_recv, o_send, o_recv, h_send, h_recv, r_send, r_recv, d_send, d_recv,
):
    s, t = lax.axis_index("sp"), lax.axis_index("tp")
    layers = wbuf.shape[0]
    rows, feat = tok.shape
    heads = feat // HEAD_DIM
    halo = REACH_R * GRID_W
    keys = rows + 2 * halo
    grid_rows = rows // GRID_W
    prev, following = lax.rem(s + n_sp - 1, n_sp), lax.rem(s + 1, n_sp)
    tp_peers = [lax.rem(t + k, n_tp) for k in range(1, n_tp)]
    sp_peers = [lax.rem(s + k, n_sp) for k in range(1, n_sp)]

    local = [
        pltpu.make_async_copy(seg, docbuf.at[1], local_sem.at[0]),
        pltpu.make_async_copy(gains, gbuf, local_sem.at[1]),
        pltpu.make_async_copy(rel, relbuf, local_sem.at[2]),
        pltpu.make_async_copy(tok, xbuf.at[0, t], local_sem.at[3]),
    ]
    weights = (wq, wk, wv)
    for l in range(layers):
        for j in range(3):
            local.append(pltpu.make_async_copy(weights[j].at[l], wbuf.at[l, j, s], local_sem.at[4 + 4 * l + j]))
        local.append(pltpu.make_async_copy(wo.at[l], wobuf.at[l, s], local_sem.at[7 + 4 * l]))
    for copy in local:
        copy.start()

    barrier = pltpu.get_barrier_semaphore()
    for peer in tp_peers:
        pl.semaphore_signal(barrier, inc=1, device_id=(s, peer), device_id_type=MESH)
    for peer in sp_peers:
        pl.semaphore_signal(barrier, inc=1, device_id=(peer, t), device_id_type=MESH)
    pl.semaphore_wait(barrier, n_tp + n_sp - 2)

    def x_copy(l, slot, peer):
        return remote(tok if l == 0 else cur, xbuf.at[l, slot], x_send.at[l, peer], x_recv.at[l, slot], (s, peer))

    def w_copy(l, j, slot, peer):
        return remote(weights[j].at[l], wbuf.at[l, j, slot], w_send.at[l, j, peer], w_recv.at[l, j, slot], (peer, t))

    def o_copy(l, slot, peer):
        return remote(wo.at[l], wobuf.at[l, slot], o_send.at[l, peer], o_recv.at[l, slot], (peer, t))

    def halo_copies(l):
        up = remote(
            kvbuf.at[l, :, pl.ds(rows, halo)], kvbuf.at[l, :, pl.ds(0, halo)],
            h_send.at[l, 0], h_recv.at[l, 0], (following, t),
        )
        down = remote(
            kvbuf.at[l, :, pl.ds(halo, halo)], kvbuf.at[l, :, pl.ds(rows + halo, halo)],
            h_send.at[l, 1], h_recv.at[l, 1], (prev, t),
        )
        return up, down

    def r_copy(l, peer, slot):
        return remote(part.at[l, peer], rsbuf.at[l, slot], r_send.at[l, peer], r_recv.at[l, slot], (s, peer))

    docs = (
        remote(seg, docbuf.at[0], d_send.at[0], d_recv.at[0], (following, t)),
        remote(seg, docbuf.at[2], d_send.at[1], d_recv.at[1], (prev, t)),
    )
    for peer in tp_peers:
        x_copy(0, t, peer).start()
    for j in (1, 2, 0):
        for peer in sp_peers:
            w_copy(0, j, s, peer).start()
    for copy in docs:
        copy.start()

    local[0].wait()
    local[1].wait()
    local[2].wait()
    for copy in docs:
        copy.wait_recv()

    doc_before = jnp.where(s == 0, -1, docbuf[0])
    doc_after = jnp.where(s == n_sp - 1, -1, docbuf[2])
    doc_own = docbuf[1]
    doc_keys = jnp.concatenate([doc_before[:, rows - halo :], doc_own, doc_after[:, :halo]], axis=1).astype(F32)
    doc_query = jnp.transpose(jnp.broadcast_to(doc_own.astype(F32), (rows, rows)))[:, :1]
    lane = lax.broadcasted_iota(jnp.int32, (1, keys), 1)
    key_row = lane // GRID_W
    key_col = lax.rem(lax.broadcasted_iota(jnp.int32, (GRID_W, keys), 1), GRID_W)
    col_off = key_col - lax.broadcasted_iota(jnp.int32, (GRID_W, keys), 0)
    for l in range(layers):
        for h in range(heads):
            table = relbuf[l, h]
            cells = [
                [jnp.broadcast_to(table[a : a + 1, b : b + 1], (1, keys)) for b in range(2 * REACH_C + 1)]
                for a in range(2 * REACH_R + 1)
            ]
            for r in range(grid_rows):
                block = jnp.full((GRID_W, keys), masked_score, F32)
                for b in range(2 * REACH_C + 1):
                    line = jnp.full((1, keys), masked_score, F32)
                    for a in range(2 * REACH_R + 1):
                        line = jnp.where(key_row == r + a, cells[a][b], line)
                    block = jnp.where(col_off == b - REACH_C, line, block)
                same = doc_query[r * GRID_W : (r + 1) * GRID_W] == doc_keys
                biasbuf[l, pl.ds(h * rows + r * GRID_W, GRID_W)] = jnp.where(same, block, masked_score)

    local[3].wait()
    for copy in local[4:]:
        copy.wait()

    for l in range(layers):
        for peer in tp_peers:
            x_copy(l, peer, peer).wait_recv()
        pieces = [xbuf[l, i].astype(F32) for i in range(n_tp)]
        square = sum(piece * piece for piece in pieces)
        mean_sq = jnp.sum(square, axis=-1, keepdims=True) / (n_tp * feat)
        inv = lax.rsqrt(mean_sq + norm_eps)
        gain = gbuf[l : l + 1]
        normed = jnp.concatenate(
            [(piece * inv * gain[:, i * feat : (i + 1) * feat]).astype(BF16) for i, piece in enumerate(pieces)],
            axis=1,
        )

        def project(j):
            for peer in sp_peers:
                w_copy(l, j, peer, peer).wait_recv()
            weight = wbuf[l, j].reshape(n_tp * feat, feat)
            return jnp.dot(normed, weight, preferred_element_type=F32).astype(BF16)

        kvbuf[l, 0, pl.ds(halo, rows)] = project(1)
        kvbuf[l, 1, pl.ds(halo, rows)] = project(2)
        halos = halo_copies(l)
        for copy in halos:
            copy.start()
        if l == 0:
            for peer in sp_peers:
                o_copy(0, s, peer).start()
        query = project(0) * jnp.asarray(HEAD_DIM**-0.5, BF16)
        head_of = lax.broadcasted_iota(jnp.int32, (rows, feat), 1) // HEAD_DIM
        query = jnp.concatenate([jnp.where(head_of == h, query, jnp.zeros_like(query)) for h in range(heads)], axis=0)
        for copy in halos:
            copy.wait_recv()
        if l + 1 < layers:
            for j in (1, 2, 0):
                for peer in sp_peers:
                    w_copy(l + 1, j, s, peer).start()
        scores = lax.dot_general(query, kvbuf[l, 0], (((1,), (1,)), ((), ())), preferred_element_type=F32)
        scores = scores + biasbuf[l]
        weight = jnp.exp(scores - jnp.max(scores, axis=-1, keepdims=True))
        total = jnp.sum(weight, axis=-1, keepdims=True)
        blended = jnp.dot(weight.astype(BF16), kvbuf[l, 1], preferred_element_type=F32) / total
        attended = blended[:rows]
        for h in range(1, heads):
            attended = jnp.where(head_of == h, blended[h * rows : (h + 1) * rows], attended)
        attended = attended.astype(BF16)

        for peer in sp_peers:
            o_copy(l, peer, peer).wait_recv()
        if l + 1 < layers:
            for peer in sp_peers:
                o_copy(l + 1, s, peer).start()
        width = wobuf.shape[3]
        for i in range(n_sp):
            piece = jnp.dot(attended, wobuf[l, i], preferred_element_type=F32).astype(BF16)
            for j in range(width // feat):
                part[l, i * (width // feat) + j] = piece[:, j * feat : (j + 1) * feat]
        for peer in tp_peers:
            r_copy(l, peer, t).start()
        summed = part[l, t].astype(F32)
        for peer in tp_peers:
            r_copy(l, peer, peer).wait_recv()
            summed = summed + rsbuf[l, peer].astype(F32)
        if l + 1 < layers:
            cur[...] = summed.astype(BF16)
            for peer in tp_peers:
                x_copy(l + 1, t, peer).start()
            xbuf[l + 1, t] = summed.astype(BF16)
        else:
            out[...] = summed.astype(BF16)

    for copy in docs:
        copy.wait_send()
    for l in range(layers):
        for peer in tp_peers:
            x_copy(l, t, peer).wait_send()
            r_copy(l, peer, t).wait_send()
        for peer in sp_peers:
            for j in range(3):
                w_copy(l, j, s, peer).wait_send()
            o_copy(l, s, peer).wait_send()
        for copy in halo_copies(l):
            copy.wait_send()


def on_device(n_sp, n_tp, tokens, segment_ids, gains, w_query, w_key, w_value, w_out, rel_bias):
    rows, feat = tokens.shape
    layers, depth, _ = w_query.shape
    width = w_out.shape[2]
    halo = REACH_R * GRID_W
    keys = rows + 2 * halo
    heads = feat // HEAD_DIM
    dma = pltpu.SemaphoreType.DMA
    anywhere = pl.BlockSpec(memory_space=pl.ANY)
    return pl.pallas_call(
        functools.partial(kernel, n_sp, n_tp),
        out_shape=jax.ShapeDtypeStruct((rows, feat), BF16),
        in_specs=[anywhere] * 8,
        out_specs=pl.BlockSpec(memory_space=pltpu.VMEM),
        scratch_shapes=[
            pltpu.VMEM((layers, n_tp, rows, feat), BF16),
            pltpu.VMEM((layers, 3, n_sp, depth, feat), BF16),
            pltpu.VMEM((layers, n_sp, feat, width), BF16),
            pltpu.VMEM((layers, 2, keys, feat), BF16),
            pltpu.VMEM((layers, n_tp, rows, feat), BF16),
            pltpu.VMEM((layers, n_tp, rows, feat), BF16),
            pltpu.VMEM((rows, feat), BF16),
            pltpu.VMEM((3, 1, rows), jnp.int32),
            pltpu.VMEM(gains.shape, F32),
            pltpu.VMEM(rel_bias.shape, F32),
            pltpu.VMEM((layers, heads * rows, keys), F32),
            dma((4 + 4 * layers,)),
            dma((layers, n_tp)),
            dma((layers, n_tp)),
            dma((layers, 3, n_sp)),
            dma((layers, 3, n_sp)),
            dma((layers, n_sp)),
            dma((layers, n_sp)),
            dma((layers, 2)),
            dma((layers, 2)),
            dma((layers, n_tp)),
            dma((layers, n_tp)),
            dma((2,)),
            dma((2,)),
        ],
        compiler_params=pltpu.CompilerParams(
            collective_id=0, has_side_effects=True, vmem_limit_bytes=48 * 1024 * 1024
        ),
    )(tokens, segment_ids.reshape(1, rows), gains, w_query, w_key, w_value, w_out, rel_bias)


def solution(mesh):
    return jax.shard_map(
        functools.partial(on_device, mesh.shape["sp"], mesh.shape["tp"]),
        mesh=mesh,
        in_specs=(
            P("sp", "tp"),
            P("sp"),
            P(),
            P(None, "sp", "tp"),
            P(None, "sp", "tp"),
            P(None, "sp", "tp"),
            P(None, "tp", "sp"),
            P(None, "tp", None, None),
        ),
        out_specs=P("sp", "tp"),
        check_vma=False,
    )
```

```python
import functools

import jax
import jax.numpy as jnp
from jax import lax
from jax.experimental import pallas as pl
from jax.experimental.pallas import tpu as pltpu
from jax.sharding import PartitionSpec as P

MESH = pl.DeviceIdType.MESH

HEAD_DIM = 64
GRID_W = 32
REACH_R = 2
REACH_C = 4

norm_eps = 1e-06
masked_score = -1e30
F32 = jnp.float32
BF16 = jnp.bfloat16


def remote(src, dst, send_sem, recv_sem, where):
    return pltpu.make_async_remote_copy(
        src_ref=src, dst_ref=dst, send_sem=send_sem, recv_sem=recv_sem, device_id=where, device_id_type=MESH
    )


def kernel(
    n_sp, n_tp, tok, seg, gains, wq, wk, wv, wo, rel, out,
    xbuf, wbuf, wobuf, kvbuf, part, rsbuf, cur, docbuf, gbuf, relbuf, biasbuf,
    local_sem, x_send, x_recv, w_send, w_recv, o_send, o_recv, h_send, h_recv, r_send, r_recv, d_send, d_recv,
):
    s, t = lax.axis_index("sp"), lax.axis_index("tp")
    layers = wbuf.shape[0]
    rows, feat = tok.shape
    heads = feat // HEAD_DIM
    halo = REACH_R * GRID_W
    keys = rows + 2 * halo
    grid_rows = rows // GRID_W
    prev, following = lax.rem(s + n_sp - 1, n_sp), lax.rem(s + 1, n_sp)
    tp_peers = [lax.rem(t + k, n_tp) for k in range(1, n_tp)]
    sp_peers = [lax.rem(s + k, n_sp) for k in range(1, n_sp)]

    local = [
        pltpu.make_async_copy(seg, docbuf.at[1], local_sem.at[0]),
        pltpu.make_async_copy(gains, gbuf, local_sem.at[1]),
        pltpu.make_async_copy(rel, relbuf, local_sem.at[2]),
        pltpu.make_async_copy(tok, xbuf.at[0, t], local_sem.at[3]),
    ]
    weights = (wq, wk, wv)
    for l in range(layers):
        for j in range(3):
            local.append(pltpu.make_async_copy(weights[j].at[l], wbuf.at[l, j, s], local_sem.at[4 + 4 * l + j]))
        local.append(pltpu.make_async_copy(wo.at[l], wobuf.at[l, s], local_sem.at[7 + 4 * l]))
    for copy in local:
        copy.start()

    barrier = pltpu.get_barrier_semaphore()
    for peer in tp_peers:
        pl.semaphore_signal(barrier, inc=1, device_id=(s, peer), device_id_type=MESH)
    for peer in sp_peers:
        pl.semaphore_signal(barrier, inc=1, device_id=(peer, t), device_id_type=MESH)
    pl.semaphore_wait(barrier, n_tp + n_sp - 2)

    def x_copy(l, slot, peer):
        return remote(tok if l == 0 else cur, xbuf.at[l, slot], x_send.at[l, peer], x_recv.at[l, slot], (s, peer))

    def w_copy(l, j, slot, peer):
        return remote(weights[j].at[l], wbuf.at[l, j, slot], w_send.at[l, j, peer], w_recv.at[l, j, slot], (peer, t))

    def o_copy(l, slot, peer):
        return remote(wo.at[l], wobuf.at[l, slot], o_send.at[l, peer], o_recv.at[l, slot], (peer, t))

    def halo_copies(l):
        up = remote(
            kvbuf.at[l, :, pl.ds(rows, halo)], kvbuf.at[l, :, pl.ds(0, halo)],
            h_send.at[l, 0], h_recv.at[l, 0], (following, t),
        )
        down = remote(
            kvbuf.at[l, :, pl.ds(halo, halo)], kvbuf.at[l, :, pl.ds(rows + halo, halo)],
            h_send.at[l, 1], h_recv.at[l, 1], (prev, t),
        )
        return up, down

    def r_copy(l, peer, slot):
        return remote(part.at[l, peer], rsbuf.at[l, slot], r_send.at[l, peer], r_recv.at[l, slot], (s, peer))

    docs = (
        remote(seg, docbuf.at[0], d_send.at[0], d_recv.at[0], (following, t)),
        remote(seg, docbuf.at[2], d_send.at[1], d_recv.at[1], (prev, t)),
    )
    for peer in tp_peers:
        x_copy(0, t, peer).start()
    for j in (1, 2, 0):
        for peer in sp_peers:
            w_copy(0, j, s, peer).start()
    for copy in docs:
        copy.start()

    local[0].wait()
    local[1].wait()
    local[2].wait()
    for copy in docs:
        copy.wait_recv()

    doc_before = jnp.where(s == 0, -1, docbuf[0])
    doc_after = jnp.where(s == n_sp - 1, -1, docbuf[2])
    doc_own = docbuf[1]
    doc_keys = jnp.concatenate([doc_before[:, rows - halo :], doc_own, doc_after[:, :halo]], axis=1).astype(F32)
    doc_query = jnp.transpose(jnp.broadcast_to(doc_own.astype(F32), (rows, rows)))[:, :1]
    lane = lax.broadcasted_iota(jnp.int32, (1, keys), 1)
    key_row = lane // GRID_W
    key_col = lax.rem(lax.broadcasted_iota(jnp.int32, (GRID_W, keys), 1), GRID_W)
    col_off = key_col - lax.broadcasted_iota(jnp.int32, (GRID_W, keys), 0)
    for l in range(layers):
        for h in range(heads):
            cells = [
                [jnp.broadcast_to(relbuf[l, a, h : h + 1, b : b + 1], (1, keys)) for b in range(2 * REACH_C + 1)]
                for a in range(2 * REACH_R + 1)
            ]
            for r in range(grid_rows):
                block = jnp.full((GRID_W, keys), masked_score, F32)
                for b in range(2 * REACH_C + 1):
                    line = jnp.full((1, keys), masked_score, F32)
                    for a in range(2 * REACH_R + 1):
                        line = jnp.where(key_row == r + a, cells[a][b], line)
                    block = jnp.where(col_off == b - REACH_C, line, block)
                same = doc_query[r * GRID_W : (r + 1) * GRID_W] == doc_keys
                biasbuf[l, pl.ds(h * rows + r * GRID_W, GRID_W)] = jnp.where(same, block, masked_score)

    local[3].wait()
    for copy in local[4:]:
        copy.wait()

    for l in range(layers):
        for peer in tp_peers:
            x_copy(l, peer, peer).wait_recv()
        pieces = [xbuf[l, i].astype(F32) for i in range(n_tp)]
        square = sum(piece * piece for piece in pieces)
        mean_sq = jnp.sum(square, axis=-1, keepdims=True) / (n_tp * feat)
        inv = lax.rsqrt(mean_sq + norm_eps)
        gain = gbuf[l : l + 1]
        normed = jnp.concatenate(
            [(piece * inv * gain[:, i * feat : (i + 1) * feat]).astype(BF16) for i, piece in enumerate(pieces)],
            axis=1,
        )

        def project(j):
            for peer in sp_peers:
                w_copy(l, j, peer, peer).wait_recv()
            weight = wbuf[l, j].reshape(n_tp * feat, feat)
            return jnp.dot(normed, weight, preferred_element_type=F32).astype(BF16)

        kvbuf[l, 0, pl.ds(halo, rows)] = project(1)
        kvbuf[l, 1, pl.ds(halo, rows)] = project(2)
        halos = halo_copies(l)
        for copy in halos:
            copy.start()
        if l == 0:
            for peer in sp_peers:
                o_copy(0, s, peer).start()
        query = project(0) * jnp.asarray(HEAD_DIM**-0.5, BF16)
        head_of = lax.broadcasted_iota(jnp.int32, (rows, feat), 1) // HEAD_DIM
        query = jnp.concatenate([jnp.where(head_of == h, query, jnp.zeros_like(query)) for h in range(heads)], axis=0)
        for copy in halos:
            copy.wait_recv()
        if l + 1 < layers:
            for j in (1, 2, 0):
                for peer in sp_peers:
                    w_copy(l + 1, j, s, peer).start()
        scores = lax.dot_general(query, kvbuf[l, 0], (((1,), (1,)), ((), ())), preferred_element_type=F32)
        scores = scores + biasbuf[l]
        weight = jnp.exp(scores - jnp.max(scores, axis=-1, keepdims=True))
        total = jnp.sum(weight, axis=-1, keepdims=True)
        blended = jnp.dot(weight.astype(BF16), kvbuf[l, 1], preferred_element_type=F32) / total
        attended = blended[:rows]
        for h in range(1, heads):
            attended = jnp.where(head_of == h, blended[h * rows : (h + 1) * rows], attended)
        attended = attended.astype(BF16)

        for peer in sp_peers:
            o_copy(l, peer, peer).wait_recv()
        if l + 1 < layers:
            for peer in sp_peers:
                o_copy(l + 1, s, peer).start()
        width = wobuf.shape[3]
        for i in range(n_sp):
            piece = jnp.dot(attended, wobuf[l, i], preferred_element_type=F32).astype(BF16)
            for j in range(width // feat):
                part[l, i * (width // feat) + j] = piece[:, j * feat : (j + 1) * feat]
        for peer in tp_peers:
            r_copy(l, peer, t).start()
        summed = part[l, t].astype(F32)
        for peer in tp_peers:
            r_copy(l, peer, peer).wait_recv()
            summed = summed + rsbuf[l, peer].astype(F32)
        if l + 1 < layers:
            cur[...] = summed.astype(BF16)
            for peer in tp_peers:
                x_copy(l + 1, t, peer).start()
            xbuf[l + 1, t] = summed.astype(BF16)
        else:
            out[...] = summed.astype(BF16)

    for copy in docs:
        copy.wait_send()
    for l in range(layers):
        for peer in tp_peers:
            x_copy(l, t, peer).wait_send()
            r_copy(l, peer, t).wait_send()
        for peer in sp_peers:
            for j in range(3):
                w_copy(l, j, s, peer).wait_send()
            o_copy(l, s, peer).wait_send()
        for copy in halo_copies(l):
            copy.wait_send()


def on_device(n_sp, n_tp, tokens, segment_ids, gains, w_query, w_key, w_value, w_out, rel_bias):
    rows, feat = tokens.shape
    layers, depth, _ = w_query.shape
    width = w_out.shape[2]
    halo = REACH_R * GRID_W
    keys = rows + 2 * halo
    heads = feat // HEAD_DIM
    rel_by_row = jnp.transpose(rel_bias, (0, 2, 1, 3))
    dma = pltpu.SemaphoreType.DMA
    anywhere = pl.BlockSpec(memory_space=pltpu.HBM)
    return pl.pallas_call(
        functools.partial(kernel, n_sp, n_tp),
        out_shape=jax.ShapeDtypeStruct((rows, feat), BF16),
        in_specs=[anywhere] * 8,
        out_specs=pl.BlockSpec(memory_space=pltpu.VMEM),
        scratch_shapes=[
            pltpu.VMEM((layers, n_tp, rows, feat), BF16),
            pltpu.VMEM((layers, 3, n_sp, depth, feat), BF16),
            pltpu.VMEM((layers, n_sp, feat, width), BF16),
            pltpu.VMEM((layers, 2, keys, feat), BF16),
            pltpu.VMEM((layers, n_tp, rows, feat), BF16),
            pltpu.VMEM((layers, n_tp, rows, feat), BF16),
            pltpu.VMEM((rows, feat), BF16),
            pltpu.VMEM((3, 1, rows), jnp.int32),
            pltpu.VMEM(gains.shape, F32),
            pltpu.VMEM(rel_by_row.shape, F32),
            pltpu.VMEM((layers, heads * rows, keys), F32),
            dma((4 + 4 * layers,)),
            dma((layers, n_tp)),
            dma((layers, n_tp)),
            dma((layers, 3, n_sp)),
            dma((layers, 3, n_sp)),
            dma((layers, n_sp)),
            dma((layers, n_sp)),
            dma((layers, 2)),
            dma((layers, 2)),
            dma((layers, n_tp)),
            dma((layers, n_tp)),
            dma((2,)),
            dma((2,)),
        ],
        compiler_params=pltpu.CompilerParams(
            collective_id=0, has_side_effects=True, vmem_limit_bytes=67043328
        ),
    )(tokens, segment_ids.reshape(1, rows), gains, w_query, w_key, w_value, w_out, rel_by_row)


def solution(mesh):
    return jax.shard_map(
        functools.partial(on_device, mesh.shape["sp"], mesh.shape["tp"]),
        mesh=mesh,
        in_specs=(
            P("sp", "tp"),
            P("sp"),
            P(),
            P(None, "sp", "tp"),
            P(None, "sp", "tp"),
            P(None, "sp", "tp"),
            P(None, "tp", "sp"),
            P(None, "tp", None, None),
        ),
        out_specs=P("sp", "tp"),
        check_vma=False,
    )
```

```python
import functools

import jax
import jax.numpy as jnp
from jax import lax
from jax.experimental import pallas as pl
from jax.experimental.pallas import tpu as pltpu
from jax.sharding import PartitionSpec as P

MESH = pl.DeviceIdType.MESH

HEAD_DIM = 64
GRID_W = 32
REACH_R = 2
REACH_C = 4

norm_eps = 1e-06
masked_score = -1e30
F32 = jnp.float32
BF16 = jnp.bfloat16


def remote(src, dst, send_sem, recv_sem, where):
    return pltpu.make_async_remote_copy(
        src_ref=src, dst_ref=dst, send_sem=send_sem, recv_sem=recv_sem, device_id=where, device_id_type=MESH
    )


def kernel(
    n_sp, n_tp, tok, seg, gains, wq, wk, wv, wo, rel, out,
    xbuf, wbuf, wobuf, kvbuf, part, rsbuf, cur, docbuf, gbuf, relbuf, biasbuf,
    local_sem, x_send, x_recv, w_send, w_recv, o_send, o_recv, h_send, h_recv, r_send, r_recv, d_send, d_recv, e_send, e_recv, f_send, f_recv,
):
    s, t = lax.axis_index("sp"), lax.axis_index("tp")
    layers = wbuf.shape[0]
    rows, feat = tok.shape
    heads = feat // HEAD_DIM
    halo = REACH_R * GRID_W
    keys = rows + 2 * halo
    grid_rows = rows // GRID_W
    prev, following = lax.rem(s + n_sp - 1, n_sp), lax.rem(s + 1, n_sp)
    tp_peers = [lax.rem(t + k, n_tp) for k in range(1, n_tp)]
    sp_peers = [lax.rem(s + k, n_sp) for k in range(1, n_sp)]

    local = [
        pltpu.make_async_copy(seg, docbuf.at[1], local_sem.at[0]),
        pltpu.make_async_copy(gains, gbuf, local_sem.at[1]),
        pltpu.make_async_copy(rel, relbuf, local_sem.at[2]),
        pltpu.make_async_copy(tok, xbuf.at[0, t, pl.ds(halo, rows)], local_sem.at[3]),
    ]
    weights = (wq, wk, wv)
    for l in range(layers):
        for j in range(3):
            local.append(pltpu.make_async_copy(weights[j].at[l], wbuf.at[l, j, s], local_sem.at[4 + 4 * l + j]))
        local.append(pltpu.make_async_copy(wo.at[l], wobuf.at[l, s], local_sem.at[7 + 4 * l]))
    for copy in local:
        copy.start()

    barrier = pltpu.get_barrier_semaphore()
    for peer in tp_peers:
        pl.semaphore_signal(barrier, inc=1, device_id=(s, peer), device_id_type=MESH)
    for peer in sp_peers:
        pl.semaphore_signal(barrier, inc=1, device_id=(peer, t), device_id_type=MESH)
    pl.semaphore_wait(barrier, n_tp + n_sp - 2)

    def x_copy(l, slot, peer):
        return remote(tok if l == 0 else cur, xbuf.at[l, slot, pl.ds(halo, rows)], x_send.at[l, peer], x_recv.at[l, slot], (s, peer))

    def w_copy(l, j, slot, peer):
        return remote(weights[j].at[l], wbuf.at[l, j, slot], w_send.at[l, j, peer], w_recv.at[l, j, slot], (peer, t))

    def o_copy(l, slot, peer):
        return remote(wo.at[l], wobuf.at[l, slot], o_send.at[l, peer], o_recv.at[l, slot], (peer, t))

    def halo_copies(l):
        up = remote(
            kvbuf.at[l, :, pl.ds(rows, halo)], kvbuf.at[l, :, pl.ds(0, halo)],
            h_send.at[l, 0], h_recv.at[l, 0], (following, t),
        )
        down = remote(
            kvbuf.at[l, :, pl.ds(halo, halo)], kvbuf.at[l, :, pl.ds(rows + halo, halo)],
            h_send.at[l, 1], h_recv.at[l, 1], (prev, t),
        )
        return up, down

    def r_copy(l, peer, slot):
        return remote(part.at[l, peer], rsbuf.at[l, slot], r_send.at[l, peer], r_recv.at[l, slot], (s, peer))

    edges = (
        remote(
            tok.at[pl.ds(rows - halo, halo)], xbuf.at[0, t, pl.ds(0, halo)],
            e_send.at[0], e_recv.at[0], (following, t),
        ),
        remote(
            tok.at[pl.ds(0, halo)], xbuf.at[0, t, pl.ds(rows + halo, halo)],
            e_send.at[1], e_recv.at[1], (prev, t),
        ),
    )

    def edge_copy(slot, side, peer):
        piece = xbuf.at[0, slot, pl.ds(side * (rows + halo), halo)]
        return remote(piece, piece, f_send.at[peer, side], f_recv.at[slot, side], (s, peer))

    docs = (
        remote(seg, docbuf.at[0], d_send.at[0], d_recv.at[0], (following, t)),
        remote(seg, docbuf.at[2], d_send.at[1], d_recv.at[1], (prev, t)),
    )
    for copy in edges + docs:
        copy.start()
    for peer in tp_peers:
        x_copy(0, t, peer).start()
    for j in (1, 2, 0):
        for peer in sp_peers:
            w_copy(0, j, s, peer).start()
    for side in range(2):
        edges[side].wait_recv()
        for peer in tp_peers:
            edge_copy(t, side, peer).start()

    local[0].wait()
    local[1].wait()
    local[2].wait()
    for copy in docs:
        copy.wait_recv()

    doc_before = jnp.where(s == 0, -1, docbuf[0])
    doc_after = jnp.where(s == n_sp - 1, -1, docbuf[2])
    doc_own = docbuf[1]
    doc_keys = jnp.concatenate([doc_before[:, rows - halo :], doc_own, doc_after[:, :halo]], axis=1).astype(F32)
    doc_query = jnp.transpose(jnp.broadcast_to(doc_own.astype(F32), (rows, rows)))[:, :1]
    lane = lax.broadcasted_iota(jnp.int32, (1, keys), 1)
    key_row = lane // GRID_W
    key_col = lax.rem(lax.broadcasted_iota(jnp.int32, (GRID_W, keys), 1), GRID_W)
    col_off = key_col - lax.broadcasted_iota(jnp.int32, (GRID_W, keys), 0)
    for l in range(layers):
        for h in range(heads):
            cells = [
                [jnp.broadcast_to(relbuf[l, a, h : h + 1, b : b + 1], (1, keys)) for b in range(2 * REACH_C + 1)]
                for a in range(2 * REACH_R + 1)
            ]
            for r in range(grid_rows):
                block = jnp.full((GRID_W, keys), masked_score, F32)
                for b in range(2 * REACH_C + 1):
                    line = jnp.full((1, keys), masked_score, F32)
                    for a in range(2 * REACH_R + 1):
                        line = jnp.where(key_row == r + a, cells[a][b], line)
                    block = jnp.where(col_off == b - REACH_C, line, block)
                same = doc_query[r * GRID_W : (r + 1) * GRID_W] == doc_keys
                biasbuf[l, pl.ds(h * rows + r * GRID_W, GRID_W)] = jnp.where(same, block, masked_score)

    local[3].wait()
    for copy in local[4:]:
        copy.wait()

    for l in range(layers):
        for peer in tp_peers:
            x_copy(l, peer, peer).wait_recv()
        if l == 0:
            for side in range(2):
                for peer in tp_peers:
                    edge_copy(peer, side, peer).wait_recv()
            first, count = 0, keys
        else:
            first, count = halo, rows
        pieces = [xbuf[l, i, pl.ds(first, count)].astype(F32) for i in range(n_tp)]
        square = sum(piece * piece for piece in pieces)
        mean_sq = jnp.sum(square, axis=-1, keepdims=True) / (n_tp * feat)
        inv = lax.rsqrt(mean_sq + norm_eps)
        gain = gbuf[l : l + 1]
        normed = jnp.concatenate(
            [(piece * inv * gain[:, i * feat : (i + 1) * feat]).astype(BF16) for i, piece in enumerate(pieces)],
            axis=1,
        )

        def project(j, features):
            for peer in sp_peers:
                w_copy(l, j, peer, peer).wait_recv()
            weight = wbuf[l, j].reshape(n_tp * feat, feat)
            return jnp.dot(features, weight, preferred_element_type=F32).astype(BF16)

        kvbuf[l, 0, pl.ds(first, count)] = project(1, normed)
        kvbuf[l, 1, pl.ds(first, count)] = project(2, normed)
        halos = halo_copies(l) if l else ()
        for copy in halos:
            copy.start()
        if l == 0:
            for peer in sp_peers:
                o_copy(0, s, peer).start()
        query = project(0, normed[halo - first : halo - first + rows]) * jnp.asarray(HEAD_DIM**-0.5, BF16)
        head_of = lax.broadcasted_iota(jnp.int32, (rows, feat), 1) // HEAD_DIM
        query = jnp.concatenate([jnp.where(head_of == h, query, jnp.zeros_like(query)) for h in range(heads)], axis=0)
        for copy in halos:
            copy.wait_recv()
        if l + 1 < layers:
            for j in (1, 2, 0):
                for peer in sp_peers:
                    w_copy(l + 1, j, s, peer).start()
        scores = lax.dot_general(query, kvbuf[l, 0], (((1,), (1,)), ((), ())), preferred_element_type=F32)
        scores = scores + biasbuf[l]
        weight = jnp.exp(scores - jnp.max(scores, axis=-1, keepdims=True))
        total = jnp.sum(weight, axis=-1, keepdims=True)
        blended = jnp.dot(weight.astype(BF16), kvbuf[l, 1], preferred_element_type=F32) / total
        attended = blended[:rows]
        for h in range(1, heads):
            attended = jnp.where(head_of == h, blended[h * rows : (h + 1) * rows], attended)
        attended = attended.astype(BF16)

        for peer in sp_peers:
            o_copy(l, peer, peer).wait_recv()
        if l + 1 < layers:
            for peer in sp_peers:
                o_copy(l + 1, s, peer).start()
        width = wobuf.shape[3]
        for i in range(n_sp):
            piece = jnp.dot(attended, wobuf[l, i], preferred_element_type=F32).astype(BF16)
            for j in range(width // feat):
                part[l, i * (width // feat) + j] = piece[:, j * feat : (j + 1) * feat]
        for peer in tp_peers:
            r_copy(l, peer, t).start()
        summed = part[l, t].astype(F32)
        for peer in tp_peers:
            r_copy(l, peer, peer).wait_recv()
            summed = summed + rsbuf[l, peer].astype(F32)
        if l + 1 < layers:
            cur[...] = summed.astype(BF16)
            for peer in tp_peers:
                x_copy(l + 1, t, peer).start()
            xbuf[l + 1, t, pl.ds(halo, rows)] = summed.astype(BF16)
        else:
            out[...] = summed.astype(BF16)

    for copy in docs:
        copy.wait_send()
    for l in range(layers):
        for peer in tp_peers:
            x_copy(l, t, peer).wait_send()
            if l == 0:
                for side in range(2):
                    edge_copy(t, side, peer).wait_send()
            r_copy(l, peer, t).wait_send()
        for peer in sp_peers:
            for j in range(3):
                w_copy(l, j, s, peer).wait_send()
            o_copy(l, s, peer).wait_send()
        for copy in halo_copies(l) if l else edges:
            copy.wait_send()


def on_device(n_sp, n_tp, tokens, segment_ids, gains, w_query, w_key, w_value, w_out, rel_bias):
    rows, feat = tokens.shape
    layers, depth, _ = w_query.shape
    width = w_out.shape[2]
    halo = REACH_R * GRID_W
    keys = rows + 2 * halo
    heads = feat // HEAD_DIM
    rel_by_row = jnp.transpose(rel_bias, (0, 2, 1, 3))
    dma = pltpu.SemaphoreType.DMA
    anywhere = pl.BlockSpec(memory_space=pltpu.HBM)
    return pl.pallas_call(
        functools.partial(kernel, n_sp, n_tp),
        out_shape=jax.ShapeDtypeStruct((rows, feat), BF16),
        in_specs=[anywhere] * 8,
        out_specs=pl.BlockSpec(memory_space=pltpu.VMEM),
        scratch_shapes=[
            pltpu.VMEM((layers, n_tp, keys, feat), BF16),
            pltpu.VMEM((layers, 3, n_sp, depth, feat), BF16),
            pltpu.VMEM((layers, n_sp, feat, width), BF16),
            pltpu.VMEM((layers, 2, keys, feat), BF16),
            pltpu.VMEM((layers, n_tp, rows, feat), BF16),
            pltpu.VMEM((layers, n_tp, rows, feat), BF16),
            pltpu.VMEM((rows, feat), BF16),
            pltpu.VMEM((3, 1, rows), jnp.int32),
            pltpu.VMEM(gains.shape, F32),
            pltpu.VMEM(rel_by_row.shape, F32),
            pltpu.VMEM((layers, heads * rows, keys), F32),
            dma((4 + 4 * layers,)),
            dma((layers, n_tp)),
            dma((layers, n_tp)),
            dma((layers, 3, n_sp)),
            dma((layers, 3, n_sp)),
            dma((layers, n_sp)),
            dma((layers, n_sp)),
            dma((layers, 2)),
            dma((layers, 2)),
            dma((layers, n_tp)),
            dma((layers, n_tp)),
            dma((2,)),
            dma((2,)),
            dma((2,)),
            dma((2,)),
            dma((n_tp, 2)),
            dma((n_tp, 2)),
        ],
        compiler_params=pltpu.CompilerParams(
            collective_id=0, has_side_effects=True, vmem_limit_bytes=67043328
        ),
    )(tokens, segment_ids.reshape(1, rows), gains, w_query, w_key, w_value, w_out, rel_by_row)


def solution(mesh):
    return jax.shard_map(
        functools.partial(on_device, mesh.shape["sp"], mesh.shape["tp"]),
        mesh=mesh,
        in_specs=(
            P("sp", "tp"),
            P("sp"),
            P(),
            P(None, "sp", "tp"),
            P(None, "sp", "tp"),
            P(None, "sp", "tp"),
            P(None, "tp", "sp"),
            P(None, "tp", None, None),
        ),
        out_specs=P("sp", "tp"),
        check_vma=False,
    )
```

```python
import functools

import jax
import jax.numpy as jnp
from jax import lax
from jax.experimental import pallas as pl
from jax.experimental.pallas import tpu as pltpu
from jax.sharding import PartitionSpec as P

MESH = pl.DeviceIdType.MESH

HEAD_DIM = 64
GRID_W = 32
REACH_R = 2
REACH_C = 4

norm_eps = 1e-06
masked_score = -1e30
F32 = jnp.float32
BF16 = jnp.bfloat16


def remote(src, dst, send_sem, recv_sem, where):
    return pltpu.make_async_remote_copy(
        src_ref=src, dst_ref=dst, send_sem=send_sem, recv_sem=recv_sem, device_id=where, device_id_type=MESH
    )


def kernel(
    n_sp, n_tp, tok, seg, gains, wq, wk, wv, wo, rel, out,
    xbuf, wbuf, wobuf, kvbuf, part, rsbuf, cur, docbuf, gbuf, relbuf, biasbuf,
    local_sem, x_send, x_recv, w_send, w_recv, o_send, o_recv, h_send, h_recv, r_send, r_recv, d_send, d_recv,
):
    s, t = lax.axis_index("sp"), lax.axis_index("tp")
    layers = wbuf.shape[0]
    rows, feat = tok.shape
    heads = feat // HEAD_DIM
    halo = REACH_R * GRID_W
    keys = rows + 2 * halo
    grid_rows = rows // GRID_W
    prev, following = lax.rem(s + n_sp - 1, n_sp), lax.rem(s + 1, n_sp)
    tp_peers = [lax.rem(t + k, n_tp) for k in range(1, n_tp)]
    other = lambda i: i + 1 - 2 * lax.rem(i, 2)
    partner = other(t)
    mates = [lax.rem(t + k, n_tp) for k in range(2, n_tp, 2)]
    sp_peers = [lax.rem(s + k, n_sp) for k in range(1, n_sp)]

    local = [
        pltpu.make_async_copy(seg, docbuf.at[1], local_sem.at[0]),
        pltpu.make_async_copy(gains, gbuf, local_sem.at[1]),
        pltpu.make_async_copy(rel, relbuf, local_sem.at[2]),
        pltpu.make_async_copy(tok, xbuf.at[0, t], local_sem.at[3]),
    ]
    weights = (wq, wk, wv)
    for l in range(layers):
        for j in range(3):
            local.append(pltpu.make_async_copy(weights[j].at[l], wbuf.at[l, j, s], local_sem.at[4 + 4 * l + j]))
        local.append(pltpu.make_async_copy(wo.at[l], wobuf.at[l, s], local_sem.at[7 + 4 * l]))
    for copy in local:
        copy.start()

    barrier = pltpu.get_barrier_semaphore()
    for peer in tp_peers:
        pl.semaphore_signal(barrier, inc=1, device_id=(s, peer), device_id_type=MESH)
    for peer in sp_peers:
        pl.semaphore_signal(barrier, inc=1, device_id=(peer, t), device_id_type=MESH)
    pl.semaphore_wait(barrier, n_tp + n_sp - 2)

    def x_copy(l, slot, peer):
        return remote(tok if l == 0 else cur, xbuf.at[l, slot], x_send.at[l, peer], x_recv.at[l, slot], (s, peer))

    def x_forward(l, slot):
        piece = xbuf.at[l, slot]
        return remote(piece, piece, x_send.at[l, other(slot)], x_recv.at[l, slot], (s, partner))

    def spread(l):
        for mate in mates:
            x_copy(l, t, mate).start()
        x_copy(l, t, partner).start()

    def pass_on(l):
        for mate in mates:
            x_copy(l, mate, mate).wait_recv()
            x_forward(l, mate).start()

    def w_copy(l, j, slot, peer):
        return remote(weights[j].at[l], wbuf.at[l, j, slot], w_send.at[l, j, peer], w_recv.at[l, j, slot], (peer, t))

    def o_copy(l, slot, peer):
        return remote(wo.at[l], wobuf.at[l, slot], o_send.at[l, peer], o_recv.at[l, slot], (peer, t))

    def halo_copies(l):
        up = remote(
            kvbuf.at[l, :, pl.ds(rows, halo)], kvbuf.at[l, :, pl.ds(0, halo)],
            h_send.at[l, 0], h_recv.at[l, 0], (following, t),
        )
        down = remote(
            kvbuf.at[l, :, pl.ds(halo, halo)], kvbuf.at[l, :, pl.ds(rows + halo, halo)],
            h_send.at[l, 1], h_recv.at[l, 1], (prev, t),
        )
        return up, down

    def r_copy(l, peer, slot):
        return remote(part.at[l, peer], rsbuf.at[l, slot], r_send.at[l, peer], r_recv.at[l, slot], (s, peer))

    docs = (
        remote(seg, docbuf.at[0], d_send.at[0], d_recv.at[0], (following, t)),
        remote(seg, docbuf.at[2], d_send.at[1], d_recv.at[1], (prev, t)),
    )
    spread(0)
    for j in (1, 2, 0):
        for peer in sp_peers:
            w_copy(0, j, s, peer).start()
    for copy in docs:
        copy.start()

    pass_on(0)

    local[0].wait()
    local[1].wait()
    local[2].wait()
    for copy in docs:
        copy.wait_recv()

    doc_before = jnp.where(s == 0, -1, docbuf[0])
    doc_after = jnp.where(s == n_sp - 1, -1, docbuf[2])
    doc_own = docbuf[1]
    doc_keys = jnp.concatenate([doc_before[:, rows - halo :], doc_own, doc_after[:, :halo]], axis=1).astype(F32)
    doc_query = jnp.transpose(jnp.broadcast_to(doc_own.astype(F32), (rows, rows)))[:, :1]
    lane = lax.broadcasted_iota(jnp.int32, (1, keys), 1)
    key_row = lane // GRID_W
    key_col = lax.rem(lax.broadcasted_iota(jnp.int32, (GRID_W, keys), 1), GRID_W)
    col_off = key_col - lax.broadcasted_iota(jnp.int32, (GRID_W, keys), 0)
    for l in range(layers):
        for h in range(heads):
            cells = [
                [jnp.broadcast_to(relbuf[l, a, h : h + 1, b : b + 1], (1, keys)) for b in range(2 * REACH_C + 1)]
                for a in range(2 * REACH_R + 1)
            ]
            for r in range(grid_rows):
                block = jnp.full((GRID_W, keys), masked_score, F32)
                for b in range(2 * REACH_C + 1):
                    line = jnp.full((1, keys), masked_score, F32)
                    for a in range(2 * REACH_R + 1):
                        line = jnp.where(key_row == r + a, cells[a][b], line)
                    block = jnp.where(col_off == b - REACH_C, line, block)
                same = doc_query[r * GRID_W : (r + 1) * GRID_W] == doc_keys
                biasbuf[l, pl.ds(h * rows + r * GRID_W, GRID_W)] = jnp.where(same, block, masked_score)

    local[3].wait()
    for copy in local[4:]:
        copy.wait()

    for l in range(layers):
        if l:
            pass_on(l)
        for slot in [partner] + [other(mate) for mate in mates]:
            x_copy(l, slot, slot).wait_recv()
        pieces = [xbuf[l, i].astype(F32) for i in range(n_tp)]
        square = sum(piece * piece for piece in pieces)
        mean_sq = jnp.sum(square, axis=-1, keepdims=True) / (n_tp * feat)
        inv = lax.rsqrt(mean_sq + norm_eps)
        gain = gbuf[l : l + 1]
        normed = jnp.concatenate(
            [(piece * inv * gain[:, i * feat : (i + 1) * feat]).astype(BF16) for i, piece in enumerate(pieces)],
            axis=1,
        )

        def project(j):
            for peer in sp_peers:
                w_copy(l, j, peer, peer).wait_recv()
            weight = wbuf[l, j].reshape(n_tp * feat, feat)
            return jnp.dot(normed, weight, preferred_element_type=F32).astype(BF16)

        kvbuf[l, 0, pl.ds(halo, rows)] = project(1)
        kvbuf[l, 1, pl.ds(halo, rows)] = project(2)
        halos = halo_copies(l)
        for copy in halos:
            copy.start()
        if l == 0:
            for peer in sp_peers:
                o_copy(0, s, peer).start()
        query = project(0) * jnp.asarray(HEAD_DIM**-0.5, BF16)
        head_of = lax.broadcasted_iota(jnp.int32, (rows, feat), 1) // HEAD_DIM
        query = jnp.concatenate([jnp.where(head_of == h, query, jnp.zeros_like(query)) for h in range(heads)], axis=0)
        for copy in halos:
            copy.wait_recv()
        if l + 1 < layers:
            for j in (1, 2, 0):
                for peer in sp_peers:
                    w_copy(l + 1, j, s, peer).start()
        scores = lax.dot_general(query, kvbuf[l, 0], (((1,), (1,)), ((), ())), preferred_element_type=F32)
        scores = scores + biasbuf[l]
        weight = jnp.exp(scores - jnp.max(scores, axis=-1, keepdims=True))
        total = jnp.sum(weight, axis=-1, keepdims=True)
        blended = jnp.dot(weight.astype(BF16), kvbuf[l, 1], preferred_element_type=F32) / total
        attended = blended[:rows]
        for h in range(1, heads):
            attended = jnp.where(head_of == h, blended[h * rows : (h + 1) * rows], attended)
        attended = attended.astype(BF16)

        for peer in sp_peers:
            o_copy(l, peer, peer).wait_recv()
        if l + 1 < layers:
            for peer in sp_peers:
                o_copy(l + 1, s, peer).start()
        width = wobuf.shape[3]
        for i in range(n_sp):
            piece = jnp.dot(attended, wobuf[l, i], preferred_element_type=F32).astype(BF16)
            for j in range(width // feat):
                part[l, i * (width // feat) + j] = piece[:, j * feat : (j + 1) * feat]
        for peer in tp_peers:
            r_copy(l, peer, t).start()
        summed = part[l, t].astype(F32)
        for peer in tp_peers:
            r_copy(l, peer, peer).wait_recv()
            summed = summed + rsbuf[l, peer].astype(F32)
        if l + 1 < layers:
            cur[...] = summed.astype(BF16)
            spread(l + 1)
            xbuf[l + 1, t] = summed.astype(BF16)
        else:
            out[...] = summed.astype(BF16)

    for copy in docs:
        copy.wait_send()
    for l in range(layers):
        for peer in tp_peers:
            r_copy(l, peer, t).wait_send()
        for mate in mates:
            x_copy(l, t, mate).wait_send()
            x_forward(l, mate).wait_send()
        x_copy(l, t, partner).wait_send()
        for peer in sp_peers:
            for j in range(3):
                w_copy(l, j, s, peer).wait_send()
            o_copy(l, s, peer).wait_send()
        for copy in halo_copies(l):
            copy.wait_send()


def on_device(n_sp, n_tp, tokens, segment_ids, gains, w_query, w_key, w_value, w_out, rel_bias):
    rows, feat = tokens.shape
    layers, depth, _ = w_query.shape
    width = w_out.shape[2]
    halo = REACH_R * GRID_W
    keys = rows + 2 * halo
    heads = feat // HEAD_DIM
    rel_by_row = jnp.transpose(rel_bias, (0, 2, 1, 3))
    dma = pltpu.SemaphoreType.DMA
    anywhere = pl.BlockSpec(memory_space=pltpu.HBM)
    return pl.pallas_call(
        functools.partial(kernel, n_sp, n_tp),
        out_shape=jax.ShapeDtypeStruct((rows, feat), BF16),
        in_specs=[anywhere] * 8,
        out_specs=pl.BlockSpec(memory_space=pltpu.VMEM),
        scratch_shapes=[
            pltpu.VMEM((layers, n_tp, rows, feat), BF16),
            pltpu.VMEM((layers, 3, n_sp, depth, feat), BF16),
            pltpu.VMEM((layers, n_sp, feat, width), BF16),
            pltpu.VMEM((layers, 2, keys, feat), BF16),
            pltpu.VMEM((layers, n_tp, rows, feat), BF16),
            pltpu.VMEM((layers, n_tp, rows, feat), BF16),
            pltpu.VMEM((rows, feat), BF16),
            pltpu.VMEM((3, 1, rows), jnp.int32),
            pltpu.VMEM(gains.shape, F32),
            pltpu.VMEM(rel_by_row.shape, F32),
            pltpu.VMEM((layers, heads * rows, keys), F32),
            dma((4 + 4 * layers,)),
            dma((layers, n_tp)),
            dma((layers, n_tp)),
            dma((layers, 3, n_sp)),
            dma((layers, 3, n_sp)),
            dma((layers, n_sp)),
            dma((layers, n_sp)),
            dma((layers, 2)),
            dma((layers, 2)),
            dma((layers, n_tp)),
            dma((layers, n_tp)),
            dma((2,)),
            dma((2,)),
        ],
        compiler_params=pltpu.CompilerParams(
            collective_id=0, has_side_effects=True, vmem_limit_bytes=67043328
        ),
    )(tokens, segment_ids.reshape(1, rows), gains, w_query, w_key, w_value, w_out, rel_by_row)


def solution(mesh):
    return jax.shard_map(
        functools.partial(on_device, mesh.shape["sp"], mesh.shape["tp"]),
        mesh=mesh,
        in_specs=(
            P("sp", "tp"),
            P("sp"),
            P(),
            P(None, "sp", "tp"),
            P(None, "sp", "tp"),
            P(None, "sp", "tp"),
            P(None, "tp", "sp"),
            P(None, "tp", None, None),
        ),
        out_specs=P("sp", "tp"),
        check_vma=False,
    )
```
